256 devices in a mesh: st: 64 (over z, x, core), tp: 4 (over y).
Axes of the slice: x: 4, y: 4, z: 8, core: 2. Of those that a mesh axis runs over, the one named last changes fastest.
Arguments:
- tokens: bfloat16 [65536, 4096], P('st'), may hold values from -6 to 6
- passage_ids: int32 [1024, 4], P('st'), may hold values from 0 to 191, as said below
- store: bfloat16 [192, 128, 4096], P('st'), may hold values from -6 to 6
- mix_gain: bfloat16 [4096], replicated, may hold values from 0.099609375 to 1.8984375
- w_query: bfloat16 [4096, 512], P(None, 'tp'), may hold values from -0.09375 to 0.09375
- w_key: bfloat16 [4096, 512], P(None, 'tp'), may hold values from -0.09375 to 0.09375
- w_value: bfloat16 [4096, 512], P(None, 'tp'), may hold values from -0.09375 to 0.09375
- w_cross_out: bfloat16 [512, 1024], P('tp'), may hold values from -0.5 to 0.5
- head_scale: float32 [4], replicated, may hold values from 1 to 4
- w_pool_in: bfloat16 [4096, 1024], P(None, 'tp'), may hold values from -0.09375 to 0.09375
- w_pool_mix: bfloat16 [4, 256, 256], replicated, may hold values from -0.375 to 0.375
- pool_scale: bfloat16 [1024], replicated, may hold values from 0.099609375 to 1.8984375
- gate_weight: float32 [1024], replicated, may hold values from -4 to 4
Outputs:
- mixed: bfloat16 [65536, 1024], P('st', 'tp')
The draws below stay inside these ranges and needn't reach their ends.
Inputs may be any that keep to these rules, and one draw needn't show every extreme that they name: `passage_ids`: passage p is held by index p // 3 of st. The 64 ids of one index of st (its aligned blocks of rows) fall on exactly 32 owners, 2 ids on each; one owner receives 2 ids from every index of st.
All inputs are finite; a program needn't handle non-finite values.
Results may differ from the reference program's by a relative error of at most 0.013.
Values may be sent and summed in bfloat16 or wider, within the bound.
No kernel may reach another device: no remote copies, remote signals or barrier semaphores. Data moves between devices by JAX's collectives and lax.ppermute only.
A program may use at most 128 MiB of HBM per device.

```python
import math
import jax
import jax.numpy as jnp
from jax import lax

D = 4096
HEADS = 4
HEAD_DIM = 128
POOL_WIDTH = 1024
POOL_GROUPS = 4
GROUP_WIDTH = 256
SEQ_LEN = 128
BLOCK = 64
NPB = 4
P_LEN = 128
PASS_DEV = 3
TOKENS = 65536
BLOCKS = 1024
PASSAGES = 192
REQ_DEV = 64
CAP = 2
N_ST = 64


def draw_passage_ids(key, part):
    hot_owner = jax.random.randint(jax.random.fold_in(key, 7), (), 0, N_ST)
    shifts = jnp.arange(N_ST).astype(jnp.int32)

    def one_device(device):
        device_key = jax.random.fold_in(key, device + 1000)
        priority = jax.random.randint(jax.random.fold_in(device_key, 1), (N_ST,), 0, 1 << 20) * N_ST + shifts
        priority = jnp.where(shifts == N_ST - 1, -3, priority)
        priority = jnp.where(shifts == N_ST // 2, jnp.minimum(priority, -2), priority)
        priority = jnp.where(shifts == (hot_owner - device) % N_ST, jnp.minimum(priority, -1), priority)
        ordering = jnp.argsort(priority, stable=True).astype(jnp.int32)
        owners = (device + ordering[jnp.arange(REQ_DEV) // CAP]) % N_ST
        first_pick = jax.random.randint(jax.random.fold_in(device_key, 2), (REQ_DEV,), 0, PASS_DEV)
        second_pick = jax.random.randint(jax.random.fold_in(device_key, 3), (REQ_DEV,), 0, PASS_DEV)
        chosen = owners * PASS_DEV + jnp.minimum(first_pick, second_pick)
        shuffle = jax.random.permutation(jax.random.fold_in(device_key, 4), REQ_DEV)
        return chosen[shuffle]
    all_ids = jax.vmap(one_device)(jnp.arange(N_ST).astype(jnp.int32))
    return all_ids.reshape(N_ST * REQ_DEV // NPB, NPB).astype(jnp.int32)


def shard_levels(rng, dims, pieces, low, largest):
    def one(axis_at, parts):
        heights = jax.random.uniform(jax.random.fold_in(jax.random.fold_in(rng, 6), axis_at), (parts,), jnp.float32, low / len(pieces), largest / len(pieces))
        return jnp.repeat(jnp.exp(heights), dims[axis_at] // parts).reshape((-1,) + (1,) * (len(dims) - axis_at - 1))

    level = one(*pieces[0])
    for cut in pieces[1:]:
        level = level * one(*cut)
    return level


def centred(rng, dims, spread, reach, split=(), kind=jnp.bfloat16):
    drawn = spread * jax.random.normal(rng, dims, jnp.float32)
    if split:
        drawn = drawn * shard_levels(rng, dims, split, -0.22, 0.18)
    return jnp.clip(drawn, -reach, reach).astype(kind)


def setup_inputs(seed: int = 0) -> dict:
    keys = jax.random.split(jax.random.key(seed), 14)
    return {
        "tokens": centred(keys[0], (TOKENS, D), 1.0, 6.0, ((0, 64),)),
        "passage_ids": draw_passage_ids(jax.random.fold_in(keys[13], 71), 0),
        "store": centred(keys[2], (PASSAGES, P_LEN, D), 1.0, 6.0, ((0, 64),)),
        "mix_gain": jnp.clip(1.0 + 0.18 * jax.random.normal(keys[3], (D,), jnp.float32), 0.099609375, 1.8984375).astype(jnp.bfloat16),
        "w_query": centred(keys[4], (D, HEADS * HEAD_DIM), D ** -0.5, 0.09375, ((1, 4),)),
        "w_key": centred(keys[5], (D, HEADS * HEAD_DIM), D ** -0.5, 0.09375, ((1, 4),)),
        "w_value": centred(keys[6], (D, HEADS * HEAD_DIM), D ** -0.5, 0.09375, ((1, 4),)),
        "w_cross_out": centred(keys[7], (HEADS * HEAD_DIM, POOL_WIDTH), HEAD_DIM ** -0.5, 0.5, ((0, 4),)),
        "head_scale": jnp.clip(jnp.exp(jax.random.uniform(keys[8], (HEADS,), jnp.float32, math.log(1.0), math.log(4.0))), 1.0, 4.0),
        "w_pool_in": centred(keys[9], (D, POOL_WIDTH), D ** -0.5, 0.09375, ((1, 4),)),
        "w_pool_mix": centred(keys[10], (POOL_GROUPS, GROUP_WIDTH, GROUP_WIDTH), GROUP_WIDTH ** -0.5, 0.375),
        "pool_scale": jnp.clip(1.0 + 0.18 * jax.random.normal(keys[11], (POOL_WIDTH,), jnp.float32), 0.099609375, 1.8984375).astype(jnp.bfloat16),
        "gate_weight": centred(keys[12], (POOL_WIDTH,), 1.0, 4.0, (), jnp.float32),
    }


EPSILON = 1e-06

def head_normalize(values):
    return values * lax.rsqrt(lax.optimization_barrier(jnp.mean(values * values, axis=-1, keepdims=True)) + EPSILON)

def normalize_rows(tokens, mix_gain):
    floats = tokens.astype(jnp.float32)
    scaled = floats * lax.rsqrt(lax.optimization_barrier(jnp.mean(floats * floats, axis=-1, keepdims=True)) + EPSILON)
    return (scaled * mix_gain.astype(jnp.float32)).astype(jnp.bfloat16)

def pool_residual(pooled_in, channel_ids):
    row_count, chan_width = pooled_in.shape
    sequences = pooled_in.astype(jnp.float32).reshape(row_count // SEQ_LEN, SEQ_LEN, chan_width)
    running = jnp.cumsum(sequences, axis=1)
    padded = jnp.concatenate([jnp.zeros((sequences.shape[0], 16, chan_width), jnp.float32), running], axis=1)
    upper_sum = padded[:, 16:]
    position = jnp.arange(SEQ_LEN).astype(jnp.int32)[None, :, None]
    result = jnp.zeros_like(sequences)
    for section_index in range(4):
        window = 2 << section_index
        lower_sum = padded[:, 16 - window:16 - window + SEQ_LEN]
        counted = jnp.minimum(position + 1, window).astype(jnp.float32)
        average = (upper_sum - lower_sum) / counted
        chosen = (channel_ids // GROUP_WIDTH == section_index)[None, None, :]
        result = jnp.where(chosen, average - sequences, result)
    return result.reshape(row_count, chan_width).astype(jnp.bfloat16)

def reference(tokens, passage_ids, store, mix_gain, w_query, w_key, w_value, w_cross_out, head_scale, w_pool_in, w_pool_mix, pool_scale, gate_weight):
    normed = normalize_rows(tokens, mix_gain)
    pooled_in = jnp.dot(normed, w_pool_in, preferred_element_type=jnp.float32).astype(jnp.bfloat16)
    residual = pool_residual(pooled_in, jnp.arange(POOL_WIDTH).astype(jnp.int32))
    grouped = residual.astype(jnp.float32).reshape(TOKENS, POOL_GROUPS, GROUP_WIDTH)
    pool_out = jnp.einsum('tgc,gce->tge', grouped, w_pool_mix.astype(jnp.float32)).reshape(TOKENS, POOL_WIDTH)
    pool_out = pool_out * pool_scale.astype(jnp.float32)
    queries = head_normalize(jnp.dot(normed, w_query, preferred_element_type=jnp.float32).reshape(TOKENS, HEADS, HEAD_DIM)).astype(jnp.bfloat16)
    flat_store = store.reshape(PASSAGES * P_LEN, D)
    passage_keys = head_normalize(jnp.dot(flat_store, w_key, preferred_element_type=jnp.float32).reshape(PASSAGES, P_LEN, HEADS, HEAD_DIM)).astype(jnp.bfloat16)
    passage_values = jnp.dot(flat_store, w_value, preferred_element_type=jnp.float32).astype(jnp.bfloat16).reshape(PASSAGES, P_LEN, HEADS, HEAD_DIM)
    scales = head_scale.astype(jnp.float32) / math.sqrt(HEAD_DIM)

    def one_block(inputs):
        block_queries, block_ids = inputs
        block_keys = passage_keys[block_ids].astype(jnp.float32)
        block_values = passage_values[block_ids].astype(jnp.float32)
        scores = jnp.einsum('qhd,jkhd->hqjk', block_queries.astype(jnp.float32), block_keys) * scales[:, None, None, None]
        weights = jnp.exp(scores)
        totals = lax.optimization_barrier(jnp.sum(weights, axis=(2, 3)))
        rounded = lax.optimization_barrier(weights.astype(jnp.bfloat16))
        partial_out = jnp.einsum('hqjk,jkhd->jqhd', rounded.astype(jnp.float32), block_values)
        partial_out = lax.optimization_barrier(partial_out.astype(jnp.bfloat16))
        summed = lax.optimization_barrier(jnp.sum(partial_out.astype(jnp.float32), axis=0))
        return (summed / jnp.transpose(totals)[:, :, None]).astype(jnp.bfloat16)
    attended = lax.map(one_block, (queries.reshape(BLOCKS, BLOCK, HEADS, HEAD_DIM), passage_ids))
    attended = attended.reshape(TOKENS, HEADS, HEAD_DIM)
    cross_sum = jnp.zeros((TOKENS, POOL_WIDTH), jnp.float32)
    for head_index in range(HEADS):
        rows_of_head = w_cross_out[head_index * HEAD_DIM:(head_index + 1) * HEAD_DIM]
        cross_term = jnp.dot(attended[:, head_index], rows_of_head, preferred_element_type=jnp.float32)
        cross_term = lax.optimization_barrier(cross_term.astype(jnp.bfloat16))
        cross_sum = cross_sum + cross_term.astype(jnp.float32)
    gate_value = jax.nn.sigmoid(pooled_in.astype(jnp.float32) * gate_weight.astype(jnp.float32))
    return (pool_out + gate_value * cross_sum).astype(jnp.bfloat16)
```

```python
import functools
import math

import jax
import jax.numpy as jnp
from jax import lax
from jax.experimental import pallas as pl
from jax.experimental.pallas import tpu as pltpu
from jax.sharding import PartitionSpec as P

HEAD_DIM = 128
GROUP_WIDTH = 256
SEQ_LEN = 128
BLOCK = 64
PASSAGE = 128
EPSILON = 1e-06

Z, X, C = 8, 4, 2
TP = 4
HELD = 3
KV_ROWS = 2 * HELD * PASSAGE
TAIL = 16
CAPACITY = 128
UNROLL = 8

F32, BF16 = jnp.float32, jnp.bfloat16
SMEM = pl.BlockSpec(memory_space=pltpu.SMEM)
VMEM = pl.BlockSpec(memory_space=pltpu.VMEM)
HBM = pl.BlockSpec(memory_space=pl.ANY)


def rank_of(z, x, core):
    return (z * X + x) * C + core


def st_moves(dz, dx, dc):
    return [
        (rank_of(z, x, c), rank_of((z + dz) % Z, (x + dx) % X, c ^ dc))
        for z in range(Z)
        for x in range(X)
        for c in range(C)
    ]


def z_shift(v, step):
    return v if step == 0 else lax.ppermute(v, "st", st_moves(step, 0, 0))


def x_shift(v, step):
    return v if step % X == 0 else lax.ppermute(v, "st", st_moves(0, step, 0))


def core_swap(v):
    return lax.ppermute(v, "st", st_moves(0, 0, 1))


def tp_shift(v, step):
    return v if step == 0 else lax.ppermute(v, "tp", [(i, (i + step) % TP) for i in range(TP)])


def head_normalize(values):
    return values * lax.rsqrt(jnp.mean(values * values, axis=-1, keepdims=True) + EPSILON)


def identity(n):
    return lax.broadcasted_iota(jnp.int32, (n, n), 0) == lax.broadcasted_iota(jnp.int32, (n, n), 1)


def kv_kernel(store, w_key, w_value, out, acc):
    step = pl.program_id(0)
    weights = jnp.concatenate([w_key[...], w_value[...]], axis=1)
    part = jnp.dot(store[...], weights, preferred_element_type=F32)

    @pl.when(step == 0)
    def _():
        acc[...] = part

    @pl.when(step > 0)
    def _():
        acc[...] += part

    @pl.when(step == pl.num_programs(0) - 1)
    def _():
        half = HELD * PASSAGE
        out[:half, :] = head_normalize(acc[:, :HEAD_DIM]).astype(BF16)
        out[half:, :] = acc[:, HEAD_DIM:].astype(BF16)


def own_passages(store, w_key, w_value, chunk=1024):
    rows, width = store.shape
    return pl.pallas_call(
        kv_kernel,
        grid=(width // chunk,),
        out_shape=jax.ShapeDtypeStruct((2 * rows, HEAD_DIM), BF16),
        in_specs=[
            pl.BlockSpec((rows, chunk), lambda i: (0, i)),
            pl.BlockSpec((chunk, HEAD_DIM), lambda i: (i, 0)),
            pl.BlockSpec((chunk, HEAD_DIM), lambda i: (i, 0)),
        ],
        out_specs=pl.BlockSpec((2 * rows, HEAD_DIM), lambda i: (0, 0)),
        scratch_shapes=[pltpu.VMEM((rows, 2 * HEAD_DIM), F32)],
    )(store, w_key, w_value)


def token_kernel(tokens, gain, id_rows, w_query, w_pool_in, w_mix, pool_scale, gate_weight, q_out, pool_out, gate_out):
    step = pl.program_id(0)
    rank = lax.axis_index("tp")
    tile = tokens.shape[0]
    x = tokens[...].astype(F32)
    inverse = lax.rsqrt(jnp.mean(x * x, axis=-1, keepdims=True) + EPSILON)
    normed = (x * inverse * gain[...]).astype(BF16)
    weights = jnp.concatenate([w_query[...], w_pool_in[...]], axis=1)
    both = jnp.dot(normed, weights, preferred_element_type=F32)
    q_out[pl.ds(pl.multiple_of(step * tile, tile), tile), :] = head_normalize(both[:, :HEAD_DIM]).astype(BF16)

    @pl.when(step == 0)
    def _():
        q_out[pl.num_programs(0) * tile :, :] = id_rows[...]

    window = lax.shift_left(2, rank)
    row = lax.broadcasted_iota(jnp.int32, (SEQ_LEN, SEQ_LEN), 0)
    col = lax.broadcasted_iota(jnp.int32, (SEQ_LEN, SEQ_LEN), 1)
    band = ((col <= row) & (col > row - window)).astype(F32).astype(BF16)
    position = lax.broadcasted_iota(jnp.int32, (SEQ_LEN, 1), 0)
    counted = jnp.minimum(position + 1, window).astype(F32)
    group = lax.broadcasted_iota(jnp.int32, (TP, GROUP_WIDTH), 0) == rank
    scale = jnp.sum(jnp.where(group, pool_scale[...], 0.0), axis=0, keepdims=True)
    gate_w = jnp.sum(jnp.where(group, gate_weight[...], 0.0), axis=0, keepdims=True)
    mix = w_mix[rank]
    for s in range(tile // SEQ_LEN):
        cut = slice(s * SEQ_LEN, (s + 1) * SEQ_LEN)
        pooled = both[cut, HEAD_DIM:].astype(BF16)
        wide = pooled.astype(F32)
        sums = jnp.dot(band, pooled, preferred_element_type=F32)
        residual = (sums / counted - wide).astype(BF16)
        pool_out[cut, :] = jnp.dot(residual, mix, preferred_element_type=F32) * scale
        gate_out[cut, :] = jax.nn.sigmoid(wide * gate_w)


def mix_tokens(tokens, gain, id_rows, w_query, w_pool_in, w_mix, pool_scale, gate_weight, tile=256):
    rows, width = tokens.shape
    full = lambda a: pl.BlockSpec(a.shape, lambda i: (0,) * a.ndim)
    return pl.pallas_call(
        token_kernel,
        grid=(rows // tile,),
        out_shape=[
            jax.ShapeDtypeStruct((rows + TAIL, HEAD_DIM), BF16),
            jax.ShapeDtypeStruct((rows, GROUP_WIDTH), F32),
            jax.ShapeDtypeStruct((rows, GROUP_WIDTH), F32),
        ],
        in_specs=[pl.BlockSpec((tile, width), lambda i: (i, 0))]
        + [full(a) for a in (gain, id_rows, w_query, w_pool_in, w_mix, pool_scale, gate_weight)],
        out_specs=[
            pl.BlockSpec((rows + TAIL, HEAD_DIM), lambda i: (0, 0)),
            pl.BlockSpec((tile, GROUP_WIDTH), lambda i: (i, 0)),
            pl.BlockSpec((tile, GROUP_WIDTH), lambda i: (i, 0)),
        ],
    )(tokens, gain, id_rows, w_query, w_pool_in, w_mix, pool_scale, gate_weight)


def pair_list(active, kv_row, rows):
    order = jnp.arange(active.shape[0])
    flags = active.astype(jnp.int32)
    before = jnp.sum(jnp.where(order[None, :] < order[:, None], flags[None, :], 0), axis=1)
    block = order // (order.shape[0] // (X * rows // BLOCK))
    hit = active[:, None] & (before[:, None] == jnp.arange(CAPACITY)[None, :])
    code = jnp.sum(jnp.where(hit, (block * 64 + kv_row + 1)[:, None], 0), axis=0)
    filled = code > 0
    code = jnp.maximum(code - 1, 0)
    blk, kv = code // 64, code % 64
    per_peer = rows // BLOCK
    query_row = (blk // per_peer) * (rows + TAIL) + (blk % per_peer) * BLOCK
    passage_row = (kv // HELD) * KV_ROWS + (kv % HELD) * PASSAGE
    sum_row = jnp.where(filled, blk * BLOCK, X * rows)
    return jnp.stack([query_row, passage_row, sum_row]), jnp.sum(flags)[None]


def attend_kernel(counts, pairs, head_scale, *refs, rows):
    queries, refs = refs[:X], refs[X:]
    chunks, refs = refs[: Z * C], refs[Z * C :]
    outs, (q_ref, kv_ref, acc, tot, sems) = refs[:X], refs[X:]
    step_rows = rows + TAIL
    copies = [
        pltpu.make_async_copy(q, q_ref.at[pl.ds(i * step_rows, step_rows), :], sems.at[i])
        for i, q in enumerate(queries)
    ] + [
        pltpu.make_async_copy(chunk, kv_ref.at[pl.ds(i * KV_ROWS, KV_ROWS), :], sems.at[X + i])
        for i, chunk in enumerate(chunks)
    ]
    for copy in copies:
        copy.start()
    acc[...] = jnp.zeros_like(acc)
    tot[...] = jnp.zeros_like(tot)
    factor = head_scale[lax.axis_index("tp")] * (1.0 / math.sqrt(HEAD_DIM))
    for copy in copies:
        copy.wait()

    def body(step, carry):
        lanes = range(UNROLL)
        at = [step * UNROLL + u for u in lanes]
        rows_kv = [pl.multiple_of(pairs[1, i], PASSAGE) for i in at]
        scores = [
            lax.dot_general(
                q_ref[pl.ds(pl.multiple_of(pairs[0, at[u]], 16), BLOCK), :],
                kv_ref[pl.ds(rows_kv[u], PASSAGE), :],
                (((1,), (1,)), ((), ())),
                preferred_element_type=F32,
            )
            for u in lanes
        ]
        e = [jnp.exp(s * factor) for s in scores]
        out = [
            jnp.dot(
                e[u].astype(BF16),
                kv_ref[pl.ds(rows_kv[u] + HELD * PASSAGE, PASSAGE), :],
                preferred_element_type=F32,
            )
            for u in lanes
        ]
        sums = [jnp.broadcast_to(jnp.sum(e[u], axis=1, keepdims=True), (BLOCK, PASSAGE)) for u in lanes]
        for u in lanes:
            to = pl.ds(pl.multiple_of(pairs[2, at[u]], BLOCK), BLOCK)
            acc[to, :] += out[u]
            tot[to, :] += sums[u]
        return carry

    lax.fori_loop(0, (counts[0] + UNROLL - 1) // UNROLL, body, 0)
    eye = identity(128).astype(F32)
    for peer, out in enumerate(outs):
        out[:rows, :] = acc[peer * rows : (peer + 1) * rows, :].astype(BF16)
        lines = [
            jnp.sum(tot[peer * rows + g * 128 : peer * rows + (g + 1) * 128, :] * eye, axis=0, keepdims=True)
            for g in range(rows // 128)
        ]
        lines.append(jnp.zeros((TAIL - rows // 128, 128), F32))
        out[rows:, :] = jnp.concatenate(lines, axis=0).astype(BF16)


def attend(counts, pairs, head_scale, queries, chunks):
    rows = queries[0].shape[0] - TAIL
    return pl.pallas_call(
        functools.partial(attend_kernel, rows=rows),
        out_shape=[jax.ShapeDtypeStruct((rows + TAIL, HEAD_DIM), BF16)] * X,
        in_specs=[SMEM, SMEM, SMEM] + [HBM] * (len(queries) + len(chunks)),
        out_specs=[VMEM] * X,
        scratch_shapes=[
            pltpu.VMEM((X * (rows + TAIL), HEAD_DIM), BF16),
            pltpu.VMEM((Z * C * KV_ROWS, HEAD_DIM), BF16),
            pltpu.VMEM((X * rows + BLOCK, HEAD_DIM), F32),
            pltpu.VMEM((X * rows + BLOCK, HEAD_DIM), F32),
            pltpu.SemaphoreType.DMA((X + Z * C,)),
        ],
    )(counts, pairs, head_scale, *queries, *chunks)


def combine_kernel(*refs):
    parts, out = refs[:X], refs[X]
    rows = out.shape[0]
    total = sum(p[rows:, :].astype(F32) for p in parts)
    eye = identity(128)
    for g in range(rows // 128):
        cut = slice(g * 128, (g + 1) * 128)
        line = jnp.broadcast_to(total[g : g + 1, :], (128, 128))
        column = jnp.sum(jnp.where(eye, line, 0.0), axis=1, keepdims=True)
        top = sum(p[cut, :].astype(F32) for p in parts)
        out[cut, :] = (top / column).astype(BF16)


def combine(parts):
    rows = parts[0].shape[0] - TAIL
    return pl.pallas_call(
        combine_kernel,
        out_shape=jax.ShapeDtypeStruct((rows, HEAD_DIM), BF16),
        in_specs=[VMEM] * X,
        out_specs=VMEM,
    )(*parts)


def output_kernel(*refs):
    heads, weights, (pool, gate, out) = refs[:TP], refs[TP : 2 * TP], refs[2 * TP :]
    left = jnp.concatenate([h[...] for h in heads], axis=1)
    right = jnp.concatenate([w[...] for w in weights], axis=0)
    cross = jnp.dot(left, right, preferred_element_type=F32)
    out[...] = (pool[...] + gate[...] * cross).astype(BF16)


def output(heads, weights, pool, gate, tile=256):
    rows = pool.shape[0]
    by_row = lambda w: pl.BlockSpec((tile, w), lambda i: (i, 0))
    return pl.pallas_call(
        output_kernel,
        grid=(rows // tile,),
        out_shape=jax.ShapeDtypeStruct(pool.shape, BF16),
        in_specs=[by_row(HEAD_DIM)] * TP
        + [pl.BlockSpec((HEAD_DIM, GROUP_WIDTH), lambda i: (0, 0))] * TP
        + [by_row(GROUP_WIDTH)] * 2,
        out_specs=by_row(GROUP_WIDTH),
    )(*heads, *weights, pool, gate)


def per_device(
    tokens,
    passage_ids,
    store,
    mix_gain,
    w_query,
    w_key,
    w_value,
    w_cross_out,
    head_scale,
    w_pool_in,
    w_pool_mix,
    pool_scale,
    gate_weight,
):
    rows = tokens.shape[0]
    slots = passage_ids.shape[1]
    rank = lax.axis_index("tp")
    st = lax.axis_index("st")
    my_z, my_x, my_core = st // (X * C), (st // C) % X, st % C

    own_kv = own_passages(store.reshape(-1, store.shape[2]), w_key, w_value)
    near = {d: z_shift(own_kv, d) for d in (0, 1, 7, 2, 6, 3, 5, 4)}
    far = {d: core_swap(near[d]) for d in near}
    chunks = [near[d] for d in range(Z)] + [far[d] for d in range(Z)]

    id_rows = jnp.pad(passage_ids.astype(BF16), ((0, 0), (0, HEAD_DIM - slots)))
    tokens, own_kv = lax.optimization_barrier((tokens, own_kv))
    own_q, pool, gate = mix_tokens(
        tokens,
        mix_gain.astype(F32).reshape(1, -1),
        id_rows,
        w_query,
        w_pool_in,
        w_pool_mix,
        pool_scale.astype(F32).reshape(TP, GROUP_WIDTH),
        gate_weight.reshape(TP, GROUP_WIDTH),
    )
    queries = [x_shift(own_q, d) for d in range(X)]

    ids = jnp.stack([q[rows:, :slots] for q in queries]).astype(jnp.int32).reshape(-1)
    owner = ids // HELD
    behind = (my_z - owner // (X * C)) % Z
    kv_row = ((owner % C != my_core) * Z + behind) * HELD + ids % HELD
    pairs, count = pair_list((owner // C) % X == my_x, kv_row, rows)

    sent = attend(count, pairs, head_scale, queries, chunks)
    back = [x_shift(s, -d) for d, s in enumerate(sent)]
    attended = combine(back)
    heads = [tp_shift(attended, d) for d in range(TP)]

    cuts = [
        lax.dynamic_slice_in_dim(w_cross_out, ((rank + d) % TP) * GROUP_WIDTH, GROUP_WIDTH, 1) for d in range(TP)
    ]
    *cuts, sent0 = lax.optimization_barrier((*cuts, sent[0]))
    weights = [tp_shift(c, d) for d, c in enumerate(cuts)]
    return output(heads, weights, pool, gate)


def solution(mesh):
    return jax.shard_map(
        per_device,
        mesh=mesh,
        in_specs=(
            P("st", None),
            P("st", None),
            P("st", None, None),
            P(),
            P(None, "tp"),
            P(None, "tp"),
            P(None, "tp"),
            P("tp", None),
            P(),
            P(None, "tp"),
            P(),
            P(),
            P(),
        ),
        out_specs=P("st", "tp"),
        check_vma=False,
    )
```

```python
import functools
import math

import jax
import jax.numpy as jnp
from jax import lax
from jax.experimental import pallas as pl
from jax.experimental.pallas import tpu as pltpu
from jax.sharding import PartitionSpec as P


HEAD_DIM = 128
GROUP_WIDTH = 256
SEQ_LEN = 128
BLOCK = 64
PASSAGE = 128
EPSILON = 1e-06

Z, X, C = 8, 4, 2
TP = 4
HELD = 3
KV_ROWS = 2 * HELD * PASSAGE
TAIL = 16
SLOTS = 4
CAPACITY = 128
HALVES = 2
UNROLL = 8

F32, BF16 = jnp.float32, jnp.bfloat16
SMEM = pl.BlockSpec(memory_space=pltpu.SMEM)
VMEM = pl.BlockSpec(memory_space=pltpu.VMEM)
HBM = pl.BlockSpec(memory_space=pl.ANY)


PARAMS = pltpu.CompilerParams(vmem_limit_bytes=20 << 20)


def in_vmem(x):
    return pltpu.with_memory_space_constraint(x, pltpu.VMEM)


def rank_of(z, x, core):
    return (z * X + x) * C + core


def st_moves(dz, dx, dc):
    return [
        (rank_of(z, x, c), rank_of((z + dz) % Z, (x + dx) % X, c ^ dc))
        for z in range(Z)
        for x in range(X)
        for c in range(C)
    ]


def z_shift(v, step):
    return v if step == 0 else lax.ppermute(v, "st", st_moves(step, 0, 0))


def x_shift(v, step):
    return v if step % X == 0 else lax.ppermute(v, "st", st_moves(0, step, 0))


def core_swap(v):
    return lax.ppermute(v, "st", st_moves(0, 0, 1))


def tp_shift(v, step):
    return v if step == 0 else lax.ppermute(v, "tp", [(i, (i + step) % TP) for i in range(TP)])


def head_normalize(values):
    return values * lax.rsqrt(jnp.mean(values * values, axis=-1, keepdims=True) + EPSILON)


def identity(n):
    return lax.broadcasted_iota(jnp.int32, (n, n), 0) == lax.broadcasted_iota(jnp.int32, (n, n), 1)


def kv_kernel(store, w_key, w_value, out, x, wk, wv, sems):
    chunks, _, chunk = x.shape
    copies = []
    for i in range(chunks):
        cut = pl.ds(i * chunk, chunk)
        copies.append(
            [
                pltpu.make_async_copy(w_key.at[cut, :], wk.at[i], sems.at[i, 0]),
                pltpu.make_async_copy(w_value.at[cut, :], wv.at[i], sems.at[i, 1]),
                pltpu.make_async_copy(store.at[:, cut], x.at[i], sems.at[i, 2]),
            ]
        )
        for copy in copies[-1]:
            copy.start()
    total = None
    for i in range(chunks):
        for copy in copies[i]:
            copy.wait()
        weights = jnp.concatenate([wk[i], wv[i]], axis=1)
        part = jnp.dot(x[i], weights, preferred_element_type=F32)
        total = part if total is None else total + part
    half = HELD * PASSAGE
    out[:half, :] = head_normalize(total[:, :HEAD_DIM]).astype(BF16)
    out[half:, :] = total[:, HEAD_DIM:].astype(BF16)


def own_passages(store, w_key, w_value, chunk=1024):
    rows, width = store.shape
    chunks = width // chunk
    return pl.pallas_call(
        kv_kernel,
        compiler_params=PARAMS,
        out_shape=pltpu.VMEM((2 * rows, HEAD_DIM), BF16),
        in_specs=[HBM] * 3,
        out_specs=VMEM,
        scratch_shapes=[
            pltpu.VMEM((chunks, rows, chunk), BF16),
            pltpu.VMEM((chunks, chunk, HEAD_DIM), BF16),
            pltpu.VMEM((chunks, chunk, HEAD_DIM), BF16),
            pltpu.SemaphoreType.DMA((chunks, 3)),
        ],
    )(*(pltpu.with_memory_space_constraint(a, pltpu.HBM) for a in (store, w_key, w_value)))


def projected(tokens, gain, weights):
    line = jnp.concatenate([gain[i : i + 1, :] for i in range(gain.shape[0])], axis=1)
    sums = jnp.dot(tokens[...] * line, weights[...], preferred_element_type=F32)
    x = tokens[...].astype(F32)
    return sums * lax.rsqrt(jnp.mean(x * x, axis=-1, keepdims=True) + EPSILON)


def query_kernel(tokens, gain, ids, w_query, out):
    step = pl.program_id(0)
    tile = tokens.shape[0]
    values = projected(tokens, gain, w_query)
    out[pl.ds(pl.multiple_of(step * tile, tile), tile), :] = head_normalize(values).astype(BF16)

    @pl.when(step == 0)
    def _():
        slots = ids.shape[1]
        lane = lax.broadcasted_iota(jnp.int32, (ids.shape[0], HEAD_DIM), 1)
        wide = jnp.zeros((ids.shape[0], HEAD_DIM), jnp.int32)
        for j in range(slots):
            wide = jnp.where(lane == j, ids[:, j : j + 1], wide)
        out[pl.num_programs(0) * tile :, :] = wide.astype(F32).astype(BF16)


def pool_kernel(tokens, gain, pool_scale, gate_weight, w_pool_in, w_mix, pool_out, gate_out):
    rank = lax.axis_index("tp")
    tile = tokens.shape[0]
    values = projected(tokens, gain, w_pool_in)
    window = lax.shift_left(2, rank)
    row = lax.broadcasted_iota(jnp.int32, (SEQ_LEN, SEQ_LEN), 0)
    col = lax.broadcasted_iota(jnp.int32, (SEQ_LEN, SEQ_LEN), 1)
    band = ((col <= row) & (col > row - window)).astype(F32).astype(BF16)
    position = lax.broadcasted_iota(jnp.int32, (SEQ_LEN, 1), 0)
    counted = jnp.minimum(position + 1, window).astype(F32)
    parts = pool_scale.shape[0] // TP

    def own(lines):
        wide = lines[...].astype(F32)
        index = lax.broadcasted_iota(jnp.int32, wide.shape, 0)
        return jnp.concatenate(
            [jnp.sum(jnp.where(index == parts * rank + i, wide, 0.0), axis=0, keepdims=True) for i in range(parts)],
            axis=1,
        )

    scale, gate_w = own(pool_scale), own(gate_weight)
    mix = w_mix[rank]
    for s in range(tile // SEQ_LEN):
        cut = slice(s * SEQ_LEN, (s + 1) * SEQ_LEN)
        pooled = values[cut, :].astype(BF16)
        wide = pooled.astype(F32)
        sums = jnp.dot(band, pooled, preferred_element_type=F32)
        residual = (sums / counted - wide).astype(BF16)
        pool_out[cut, :] = jnp.dot(residual, mix, preferred_element_type=F32) * scale
        gate_out[cut, :] = jax.nn.sigmoid(wide * gate_w)


def over_rows(kernel, tokens, others, out_shape, out_specs, tile=256):
    full = lambda a: pl.BlockSpec(a.shape, lambda i: (0,) * a.ndim)
    return pl.pallas_call(
        kernel,
        compiler_params=PARAMS,
        grid=(tokens.shape[0] // tile,),
        out_shape=out_shape,
        in_specs=[pl.BlockSpec((tile, tokens.shape[1]), lambda i: (i, 0))] + [full(a) for a in others],
        out_specs=out_specs(tile),
    )(tokens, *others)


def make_queries(tokens, gain, ids, w_query):
    shape = (tokens.shape[0] + TAIL, HEAD_DIM)
    out_specs = lambda tile: pl.BlockSpec(shape, lambda i: (0, 0))
    return over_rows(query_kernel, tokens, (gain, ids, w_query), pltpu.VMEM(shape, BF16), out_specs)


def mix_pools(tokens, gain, pool_scale, gate_weight, w_pool_in, w_mix):
    shape = pltpu.VMEM((tokens.shape[0], GROUP_WIDTH), F32)
    out_specs = lambda tile: [pl.BlockSpec((tile, GROUP_WIDTH), lambda i: (i, 0))] * 2
    return over_rows(pool_kernel, tokens, (gain, pool_scale, gate_weight, w_pool_in, w_mix), [shape, shape], out_specs)


def attend_kernel(head_scale, *refs):
    queries, refs = refs[:X], refs[X:]
    chunks, refs = refs[: Z * C], refs[Z * C :]
    outs, (q_ref, kv_ref, acc, tot, codes, codes_s, listed_kv, listed_row, sem) = refs[: X * HALVES], refs[X * HALVES :]
    full = (q_ref.shape[0] - BLOCK) // X
    rows = full - TAIL
    blocks = rows // BLOCK
    st = lax.axis_index("st")
    my_z, my_x, my_core = lax.shift_right_logical(st, 3), lax.shift_right_logical(st, 1) & 3, st & 1
    for i, q in enumerate(queries):
        q_ref[i * full : (i + 1) * full, :] = q[...]
        ids = q[pl.ds(rows, blocks), :].astype(F32).astype(jnp.int32)
        owner = lax.shift_right_logical(ids * 171, 9)
        behind = (my_z - lax.shift_right_logical(owner, 3)) & 7
        held = jnp.where((owner & 1) == my_core, 0, Z) + behind
        passage_row = held * KV_ROWS + (ids - owner * HELD) * PASSAGE
        mine = (lax.shift_right_logical(owner, 1) & 3) == my_x
        codes[i * blocks : (i + 1) * blocks, :] = jnp.where(mine, passage_row, -1)
    to_scalars = pltpu.make_async_copy(codes, codes_s, sem)
    to_scalars.start()
    acc[...] = jnp.zeros_like(acc)
    tot[...] = jnp.zeros_like(tot)
    q_ref[X * full :, :] = jnp.zeros((BLOCK, HEAD_DIM), BF16)
    for i, chunk in enumerate(chunks):
        kv_ref[i * KV_ROWS : (i + 1) * KV_ROWS, :] = chunk[...]
    to_scalars.wait()

    def list_block(at, count):
        for j in range(SLOTS):
            code = codes_s[at, j]
            listed_kv[count] = jnp.maximum(code, 0)
            listed_row[count] = at
            count += (code >= 0).astype(jnp.int32)
        return count

    count = lax.fori_loop(0, X * blocks, list_block, jnp.int32(0))
    for u in range(UNROLL):
        listed_kv[count + u] = 0
        listed_row[count + u] = X * blocks
    factor = head_scale[lax.axis_index("tp")] * (1.0 / math.sqrt(HEAD_DIM))

    def body(step, carry):
        lanes = range(UNROLL)
        at = [step * UNROLL + u for u in lanes]
        rows_kv = [pl.multiple_of(listed_kv[i], PASSAGE) for i in at]
        block = [listed_row[i] for i in at]
        rows_q = [pl.multiple_of(b * BLOCK + lax.shift_right_logical(b, 4) * TAIL, 16) for b in block]
        scores = [
            lax.dot_general(
                q_ref[pl.ds(rows_q[u], BLOCK), :],
                kv_ref[pl.ds(rows_kv[u], PASSAGE), :],
                (((1,), (1,)), ((), ())),
                preferred_element_type=F32,
            )
            for u in lanes
        ]
        e = [jnp.exp(s * factor) for s in scores]
        out = [
            jnp.dot(
                e[u].astype(BF16),
                kv_ref[pl.ds(rows_kv[u] + HELD * PASSAGE, PASSAGE), :],
                preferred_element_type=F32,
            )
            for u in lanes
        ]
        sums = [jnp.broadcast_to(jnp.sum(e[u], axis=1, keepdims=True), (BLOCK, PASSAGE)) for u in lanes]
        for u in lanes:
            to = pl.ds(pl.multiple_of(block[u] * BLOCK, BLOCK), BLOCK)
            acc[to, :] += out[u]
            tot[to, :] += sums[u]
        return carry

    lax.fori_loop(0, (count + UNROLL - 1) // UNROLL, body, 0)
    eye = identity(128).astype(F32)
    part_rows = rows // HALVES
    for i, out in enumerate(outs):
        base = i * part_rows
        out[:part_rows, :] = acc[base : base + part_rows, :].astype(BF16)
        lines = [
            jnp.sum(tot[base + g * 128 : base + (g + 1) * 128, :] * eye, axis=0, keepdims=True)
            for g in range(part_rows // 128)
        ]
        lines.append(jnp.zeros((TAIL - part_rows // 128, 128), F32))
        out[part_rows:, :] = jnp.concatenate(lines, axis=0).astype(BF16)


def attend(head_scale, queries, chunks):
    full = queries[0].shape[0]
    rows = full - TAIL
    outs = pl.pallas_call(
        attend_kernel,
        compiler_params=PARAMS,
        out_shape=[pltpu.VMEM((rows // HALVES + TAIL, HEAD_DIM), BF16)] * (X * HALVES),
        in_specs=[SMEM] + [VMEM] * (len(queries) + len(chunks)),
        out_specs=[VMEM] * (X * HALVES),
        scratch_shapes=[
            pltpu.VMEM((X * full + BLOCK, HEAD_DIM), BF16),
            pltpu.VMEM((Z * C * KV_ROWS, HEAD_DIM), BF16),
            pltpu.VMEM((X * rows + BLOCK, HEAD_DIM), F32),
            pltpu.VMEM((X * rows + BLOCK, HEAD_DIM), F32),
            pltpu.VMEM((X * rows // BLOCK, HEAD_DIM), jnp.int32),
            pltpu.SMEM((X * rows // BLOCK, HEAD_DIM), jnp.int32),
            pltpu.SMEM((CAPACITY + UNROLL,), jnp.int32),
            pltpu.SMEM((CAPACITY + UNROLL,), jnp.int32),
            pltpu.SemaphoreType.DMA(()),
        ],
    )(head_scale, *map(in_vmem, queries), *map(in_vmem, chunks))
    return [[outs[d * HALVES + part] for d in range(X)] for part in range(HALVES)]


def combined(parts, out):
    rows = parts[0].shape[0] - TAIL
    total = sum(p[rows:, :].astype(F32) for p in parts)
    eye = identity(128)
    for g in range(rows // 128):
        cut = slice(g * 128, (g + 1) * 128)
        line = jnp.broadcast_to(total[g : g + 1, :], (128, 128))
        column = jnp.sum(jnp.where(eye, line, 0.0), axis=1, keepdims=True)
        top = sum(p[cut, :].astype(F32) for p in parts)
        out[cut, :] = (top / column).astype(BF16)


def first_combine_kernel(*refs):
    parts, w_cross, outs = refs[:X], refs[X], refs[X + 1 :]
    rows = parts[0].shape[0] - TAIL
    combined(parts, outs[0])
    rank = lax.axis_index("tp")
    for d, out in enumerate(outs):
        if d:
            out[:rows, :] = outs[0][:rows, :]
        column = pl.multiple_of(((rank + d) & (TP - 1)) * GROUP_WIDTH, GROUP_WIDTH)
        out[rows : rows + HEAD_DIM, :] = w_cross[:, pl.ds(column, 128)]
        out[rows + HEAD_DIM :, :] = w_cross[:, pl.ds(column + 128, 128)]


def combine_kernel(*refs):
    combined(refs[:X], refs[X])


def combine(parts, w_cross=None):
    rows = parts[0].shape[0] - TAIL
    parts = [in_vmem(p) for p in parts]
    if w_cross is None:
        shape = pltpu.VMEM((rows, HEAD_DIM), BF16)
        return [pl.pallas_call(
            combine_kernel, compiler_params=PARAMS, out_shape=shape, in_specs=[VMEM] * X, out_specs=VMEM
        )(*parts)] * TP
    return pl.pallas_call(
        first_combine_kernel,
        compiler_params=PARAMS,
        out_shape=[pltpu.VMEM((rows + 2 * HEAD_DIM, HEAD_DIM), BF16)] * TP,
        in_specs=[VMEM] * (X + 1),
        out_specs=[VMEM] * TP,
    )(*parts, in_vmem(w_cross))


def output_kernel(*refs, part):
    heads, weights, (pool, gate) = refs[:TP], refs[TP : 2 * TP], refs[2 * TP : 2 * TP + 2]
    out, staged, sem = refs[-3:]
    rows = staged.shape[0]
    left = jnp.concatenate([h[:rows, :] for h in heads], axis=1)
    base = weights[0].shape[0] - 2 * HEAD_DIM
    right = [jnp.concatenate([w[base + i * HEAD_DIM : base + (i + 1) * HEAD_DIM, :] for w in weights], axis=0) for i in range(2)]
    cross = jnp.dot(left, jnp.concatenate(right, axis=1), preferred_element_type=F32)
    own = slice(part * rows, (part + 1) * rows)
    staged[...] = (pool[own, :] + gate[own, :] * cross).astype(BF16)
    copy = pltpu.make_async_copy(staged, out.at[pl.ds(part * rows, rows), :], sem)
    copy.start()
    copy.wait()


def output(heads, weights, pool, gate, part, before=None):
    rows = pool.shape[0] // HALVES
    operands = [in_vmem(a) for a in (*heads, *weights, pool, gate)]
    in_specs = [VMEM] * len(operands)
    aliases = {}
    if before is not None:
        aliases = {len(operands): 0}
        operands.append(before)
        in_specs.append(HBM)
    return pl.pallas_call(
        functools.partial(output_kernel, part=part),
        compiler_params=PARAMS,
        out_shape=jax.ShapeDtypeStruct(pool.shape, BF16),
        in_specs=in_specs,
        out_specs=HBM,
        scratch_shapes=[pltpu.VMEM((rows, GROUP_WIDTH), BF16), pltpu.SemaphoreType.DMA(())],
        input_output_aliases=aliases,
    )(*operands)


def per_device(
    tokens,
    passage_ids,
    store,
    mix_gain,
    w_query,
    w_key,
    w_value,
    w_cross_out,
    head_scale,
    w_pool_in,
    w_pool_mix,
    pool_scale,
    gate_weight,
):
    gain, scales, gates = (a.reshape(-1, 128) for a in (mix_gain, pool_scale, gate_weight))

    own_kv = own_passages(store.reshape(-1, store.shape[2]), w_key, w_value)
    near = {0: own_kv}
    for d in (1, 7, 2, 6):
        near[d] = z_shift(own_kv, d)

    tokens, own_kv = lax.optimization_barrier((tokens, own_kv))
    own_q = make_queries(tokens, gain, passage_ids, w_query)
    queries = [own_q]
    for d in range(1, X):
        queries.append(x_shift(own_q, d))
    for d, via, step in ((3, 2, 1), (5, 6, 7), (4, 2, 2)):
        near[d] = z_shift(near[via], step)
    chunks = [near[d] for d in range(Z)]
    for d in range(Z):
        chunks.append(core_swap(near[d]))

    sent = attend(head_scale, queries, chunks)
    back = []
    for part in range(HALVES):
        back.append([])
        for d in range(X):
            back[part].append(x_shift(sent[part][d], -d))
    tokens, w_pool_in, first = lax.optimization_barrier((tokens, w_pool_in, sent[0][0]))
    back[0][0] = first
    pool, gate = mix_pools(tokens, gain, scales, gates, w_pool_in, w_pool_mix)
    out, weights = None, None
    for part in range(HALVES):
        attended = combine(back[part], w_cross_out if part == 0 else None)
        heads = []
        for d in range(TP):
            heads.append(tp_shift(attended[d], d))
        weights = weights or heads
        out = output(heads, weights, pool, gate, part, out)
    return out


def solution(mesh):
    return jax.shard_map(
        per_device,
        mesh=mesh,
        in_specs=(
            P("st", None),
            P("st", None),
            P("st", None, None),
            P(),
            P(None, "tp"),
            P(None, "tp"),
            P(None, "tp"),
            P("tp", None),
            P(),
            P(None, "tp"),
            P(),
            P(),
            P(),
        ),
        out_specs=P("st", "tp"),
        check_vma=False,
    )
```

```python
import functools
import math

import jax
import jax.numpy as jnp
from jax import lax
from jax.experimental import pallas as pl
from jax.experimental.pallas import tpu as pltpu
from jax.sharding import PartitionSpec as P


HEAD_DIM = 128
GROUP_WIDTH = 256
SEQ_LEN = 128
BLOCK = 64
PASSAGE = 128
EPSILON = 1e-06

Z, X, C = 8, 4, 2
TP = 4
HELD = 3
KV_ROWS = 2 * HELD * PASSAGE
TAIL = 16
QUERY_TILES = ((0, 128), (128, 128), (256, 256), (512, 256), (768, 256))
SLOTS = 4
CAPACITY = 128
HALVES = 2
UNROLL = 16

F32, BF16 = jnp.float32, jnp.bfloat16
SMEM = pl.BlockSpec(memory_space=pltpu.SMEM)
VMEM = pl.BlockSpec(memory_space=pltpu.VMEM)
HBM = pl.BlockSpec(memory_space=pl.ANY)


PARAMS = pltpu.CompilerParams(vmem_limit_bytes=20 << 20)


def in_vmem(x):
    return pltpu.with_memory_space_constraint(x, pltpu.VMEM)


def rank_of(z, x, core):
    return (z * X + x) * C + core


def st_moves(dz, dx, dc):
    return [
        (rank_of(z, x, c), rank_of((z + dz) % Z, (x + dx) % X, c ^ dc))
        for z in range(Z)
        for x in range(X)
        for c in range(C)
    ]


def z_shift(v, step):
    return v if step == 0 else lax.ppermute(v, "st", st_moves(step, 0, 0))


def x_shift(v, step):
    return v if step % X == 0 else lax.ppermute(v, "st", st_moves(0, step, 0))


def core_swap(v):
    return lax.ppermute(v, "st", st_moves(0, 0, 1))


def tp_shift(v, step):
    return v if step == 0 else lax.ppermute(v, "tp", [(i, (i + step) % TP) for i in range(TP)])


def head_normalize(values):
    return values * lax.rsqrt(jnp.mean(values * values, axis=-1, keepdims=True) + EPSILON)


def identity(n):
    return lax.broadcasted_iota(jnp.int32, (n, n), 0) == lax.broadcasted_iota(jnp.int32, (n, n), 1)


def kv_kernel(store, w_key, w_value, out, x, wk, wv, sems):
    chunks, _, chunk = x.shape
    copies = []
    for i in range(chunks):
        cut = pl.ds(i * chunk, chunk)
        copies.append(
            [
                pltpu.make_async_copy(w_key.at[cut, :], wk.at[i], sems.at[i, 0]),
                pltpu.make_async_copy(w_value.at[cut, :], wv.at[i], sems.at[i, 1]),
                pltpu.make_async_copy(store.at[:, cut], x.at[i], sems.at[i, 2]),
            ]
        )
        for copy in copies[-1]:
            copy.start()
    total = None
    for i in range(chunks):
        for copy in copies[i]:
            copy.wait()
        weights = jnp.concatenate([wk[i], wv[i]], axis=1)
        part = jnp.dot(x[i], weights, preferred_element_type=F32)
        total = part if total is None else total + part
    half = HELD * PASSAGE
    out[:half, :] = head_normalize(total[:, :HEAD_DIM]).astype(BF16)
    out[half:, :] = total[:, HEAD_DIM:].astype(BF16)


def own_passages(store, w_key, w_value, chunk=1024):
    rows, width = store.shape
    chunks = width // chunk
    return pl.pallas_call(
        kv_kernel,
        compiler_params=PARAMS,
        out_shape=pltpu.VMEM((2 * rows, HEAD_DIM), BF16),
        in_specs=[HBM] * 3,
        out_specs=VMEM,
        scratch_shapes=[
            pltpu.VMEM((chunks, rows, chunk), BF16),
            pltpu.VMEM((chunks, chunk, HEAD_DIM), BF16),
            pltpu.VMEM((chunks, chunk, HEAD_DIM), BF16),
            pltpu.SemaphoreType.DMA((chunks, 3)),
        ],
    )(*(pltpu.with_memory_space_constraint(a, pltpu.HBM) for a in (store, w_key, w_value)))


def projected(tokens, gain, weights):
    line = jnp.concatenate([gain[i : i + 1, :] for i in range(gain.shape[0])], axis=1)
    sums = jnp.dot(tokens * line, weights[...], preferred_element_type=F32)
    x = tokens.astype(F32)
    return sums * lax.rsqrt(jnp.mean(x * x, axis=-1, keepdims=True) + EPSILON)


def query_kernel(tokens, gain, ids, w_query, out, t, sems):
    rows = tokens.shape[0]
    copies = [
        pltpu.make_async_copy(tokens.at[pl.ds(at, size), :], t.at[pl.ds(at, size), :], sems.at[i])
        for i, (at, size) in enumerate(QUERY_TILES)
    ]
    for copy in copies:
        copy.start()
    lane = lax.broadcasted_iota(jnp.int32, (ids.shape[0], HEAD_DIM), 1)
    wide = jnp.zeros((ids.shape[0], HEAD_DIM), jnp.int32)
    for j in range(ids.shape[1]):
        wide = jnp.where(lane == j, ids[:, j : j + 1], wide)
    out[rows:, :] = wide.astype(F32).astype(BF16)
    for copy, (at, size) in zip(copies, QUERY_TILES):
        copy.wait()
        values = projected(t[at : at + size, :], gain, w_query)
        out[at : at + size, :] = head_normalize(values).astype(BF16)


def pool_kernel(tokens, gain, pool_scale, gate_weight, w_pool_in, w_mix, pool_out, gate_out):
    rank = lax.axis_index("tp")
    tile = tokens.shape[0]
    values = projected(tokens[...], gain, w_pool_in)
    window = lax.shift_left(2, rank)
    row = lax.broadcasted_iota(jnp.int32, (SEQ_LEN, SEQ_LEN), 0)
    col = lax.broadcasted_iota(jnp.int32, (SEQ_LEN, SEQ_LEN), 1)
    band = ((col <= row) & (col > row - window)).astype(F32).astype(BF16)
    position = lax.broadcasted_iota(jnp.int32, (SEQ_LEN, 1), 0)
    counted = jnp.minimum(position + 1, window).astype(F32)
    parts = pool_scale.shape[0] // TP

    def own(lines):
        wide = lines[...].astype(F32)
        index = lax.broadcasted_iota(jnp.int32, wide.shape, 0)
        return jnp.concatenate(
            [jnp.sum(jnp.where(index == parts * rank + i, wide, 0.0), axis=0, keepdims=True) for i in range(parts)],
            axis=1,
        )

    scale, gate_w = own(pool_scale), own(gate_weight)
    mix = w_mix[rank]
    for s in range(tile // SEQ_LEN):
        cut = slice(s * SEQ_LEN, (s + 1) * SEQ_LEN)
        pooled = values[cut, :].astype(BF16)
        wide = pooled.astype(F32)
        sums = jnp.dot(band, pooled, preferred_element_type=F32)
        residual = (sums / counted - wide).astype(BF16)
        pool_out[cut, :] = jnp.dot(residual, mix, preferred_element_type=F32) * scale
        gate_out[cut, :] = jax.nn.sigmoid(wide * gate_w)


def over_rows(kernel, tokens, others, out_shape, out_specs, tile=256):
    full = lambda a: pl.BlockSpec(a.shape, lambda i: (0,) * a.ndim)
    return pl.pallas_call(
        kernel,
        compiler_params=PARAMS,
        grid=(tokens.shape[0] // tile,),
        out_shape=out_shape,
        in_specs=[pl.BlockSpec((tile, tokens.shape[1]), lambda i: (i, 0))] + [full(a) for a in others],
        out_specs=out_specs(tile),
    )(tokens, *others)


def make_queries(tokens, gain, ids, w_query):
    return pl.pallas_call(
        query_kernel,
        compiler_params=PARAMS,
        cost_estimate=pl.CostEstimate(flops=1_100_000_000, bytes_accessed=10_000_000, transcendentals=2_000),
        out_shape=pltpu.VMEM((tokens.shape[0] + TAIL, HEAD_DIM), BF16),
        in_specs=[HBM] + [VMEM] * 3,
        out_specs=VMEM,
        scratch_shapes=[pltpu.VMEM(tokens.shape, BF16), pltpu.SemaphoreType.DMA((len(QUERY_TILES),))],
    )(pltpu.with_memory_space_constraint(tokens, pltpu.HBM), gain, ids, in_vmem(w_query))


def mix_pools(tokens, gain, pool_scale, gate_weight, w_pool_in, w_mix):
    shape = pltpu.VMEM((tokens.shape[0], GROUP_WIDTH), F32)
    out_specs = lambda tile: [pl.BlockSpec((tile, GROUP_WIDTH), lambda i: (i, 0))] * 2
    return over_rows(pool_kernel, tokens, (gain, pool_scale, gate_weight, w_pool_in, w_mix), [shape, shape], out_specs)


def attend_kernel(head_scale, *refs):
    queries, refs = refs[:X], refs[X:]
    chunks, refs = refs[: Z * C], refs[Z * C :]
    outs, (q_ref, kv_ref, acc, tot, codes, codes_s, listed_kv, listed_row, sem) = refs[: X * HALVES], refs[X * HALVES :]
    full = (q_ref.shape[0] - BLOCK) // X
    rows = full - TAIL
    blocks = rows // BLOCK
    st = lax.axis_index("st")
    my_z, my_x, my_core = lax.shift_right_logical(st, 3), lax.shift_right_logical(st, 1) & 3, st & 1
    for i, q in enumerate(queries):
        q_ref[i * full : (i + 1) * full, :] = q[...]
        ids = q[pl.ds(rows, blocks), :].astype(F32).astype(jnp.int32)
        owner = lax.shift_right_logical(ids * 171, 9)
        behind = (my_z - lax.shift_right_logical(owner, 3)) & 7
        held = jnp.where((owner & 1) == my_core, 0, Z) + behind
        passage_row = held * KV_ROWS + (ids - owner * HELD) * PASSAGE
        mine = (lax.shift_right_logical(owner, 1) & 3) == my_x
        codes[i * blocks : (i + 1) * blocks, :] = jnp.where(mine, passage_row, -1)
    to_scalars = pltpu.make_async_copy(codes, codes_s, sem)
    to_scalars.start()
    acc[...] = jnp.zeros_like(acc)
    tot[...] = jnp.zeros_like(tot)
    q_ref[X * full :, :] = jnp.zeros((BLOCK, HEAD_DIM), BF16)
    for i, chunk in enumerate(chunks):
        kv_ref[i * KV_ROWS : (i + 1) * KV_ROWS, :] = chunk[...]
    to_scalars.wait()

    def list_block(at, count):
        for j in range(SLOTS):
            code = codes_s[at, j]
            listed_kv[count] = jnp.maximum(code, 0)
            listed_row[count] = at
            count += (code >= 0).astype(jnp.int32)
        return count

    count = lax.fori_loop(0, X * blocks, list_block, jnp.int32(0))
    for u in range(UNROLL):
        listed_kv[count + u] = 0
        listed_row[count + u] = X * blocks
    factor = head_scale[lax.axis_index("tp")] * (1.0 / math.sqrt(HEAD_DIM))

    def body(step, carry):
        lanes = range(UNROLL)
        at = [step * UNROLL + u for u in lanes]
        rows_kv = [pl.multiple_of(listed_kv[i], PASSAGE) for i in at]
        block = [listed_row[i] for i in at]
        rows_q = [pl.multiple_of(b * BLOCK + lax.shift_right_logical(b, 4) * TAIL, 16) for b in block]
        scores = [
            lax.dot_general(
                q_ref[pl.ds(rows_q[u], BLOCK), :],
                kv_ref[pl.ds(rows_kv[u], PASSAGE), :],
                (((1,), (1,)), ((), ())),
                preferred_element_type=F32,
            )
            for u in lanes
        ]
        e = [jnp.exp(s * factor) for s in scores]
        out = [
            jnp.dot(
                e[u].astype(BF16),
                kv_ref[pl.ds(rows_kv[u] + HELD * PASSAGE, PASSAGE), :],
                preferred_element_type=F32,
            )
            for u in lanes
        ]
        sums = [jnp.broadcast_to(jnp.sum(e[u], axis=1, keepdims=True), (BLOCK, PASSAGE)) for u in lanes]
        for u in lanes:
            to = pl.ds(pl.multiple_of(block[u] * BLOCK, BLOCK), BLOCK)
            acc[to, :] += out[u]
            tot[to, :] += sums[u]
        return carry

    lax.fori_loop(0, (count + UNROLL - 1) // UNROLL, body, 0)
    eye = identity(128).astype(F32)
    part_rows = rows // HALVES
    for i, out in enumerate(outs):
        base = i * part_rows
        out[:part_rows, :] = acc[base : base + part_rows, :].astype(BF16)
        lines = [
            jnp.sum(tot[base + g * 128 : base + (g + 1) * 128, :] * eye, axis=0, keepdims=True)
            for g in range(part_rows // 128)
        ]
        lines.append(jnp.zeros((TAIL - part_rows // 128, 128), F32))
        out[part_rows:, :] = jnp.concatenate(lines, axis=0).astype(BF16)


def attend(head_scale, queries, chunks):
    full = queries[0].shape[0]
    rows = full - TAIL
    outs = pl.pallas_call(
        attend_kernel,
        compiler_params=PARAMS,
        cost_estimate=pl.CostEstimate(flops=3_000_000_000, bytes_accessed=12_000_000, transcendentals=2_000_000),
        out_shape=[pltpu.VMEM((rows // HALVES + TAIL, HEAD_DIM), BF16)] * (X * HALVES),
        in_specs=[SMEM] + [VMEM] * (len(queries) + len(chunks)),
        out_specs=[VMEM] * (X * HALVES),
        scratch_shapes=[
            pltpu.VMEM((X * full + BLOCK, HEAD_DIM), BF16),
            pltpu.VMEM((Z * C * KV_ROWS, HEAD_DIM), BF16),
            pltpu.VMEM((X * rows + BLOCK, HEAD_DIM), F32),
            pltpu.VMEM((X * rows + BLOCK, HEAD_DIM), F32),
            pltpu.VMEM((X * rows // BLOCK, HEAD_DIM), jnp.int32),
            pltpu.SMEM((X * rows // BLOCK, HEAD_DIM), jnp.int32),
            pltpu.SMEM((CAPACITY + UNROLL,), jnp.int32),
            pltpu.SMEM((CAPACITY + UNROLL,), jnp.int32),
            pltpu.SemaphoreType.DMA(()),
        ],
    )(head_scale, *map(in_vmem, queries), *map(in_vmem, chunks))
    return [[outs[d * HALVES + part] for d in range(X)] for part in range(HALVES)]


def combined(parts, out):
    rows = parts[0].shape[0] - TAIL
    total = sum(p[rows:, :].astype(F32) for p in parts)
    eye = identity(128)
    for g in range(rows // 128):
        cut = slice(g * 128, (g + 1) * 128)
        line = jnp.broadcast_to(total[g : g + 1, :], (128, 128))
        column = jnp.sum(jnp.where(eye, line, 0.0), axis=1, keepdims=True)
        top = sum(p[cut, :].astype(F32) for p in parts)
        out[cut, :] = (top / column).astype(BF16)


def first_combine_kernel(*refs):
    parts, w_cross, outs = refs[:X], refs[X], refs[X + 1 :]
    rows = parts[0].shape[0] - TAIL
    combined(parts, outs[0])
    rank = lax.axis_index("tp")
    for d, out in enumerate(outs):
        if d:
            out[:rows, :] = outs[0][:rows, :]
        column = pl.multiple_of(((rank + d) & (TP - 1)) * GROUP_WIDTH, GROUP_WIDTH)
        out[rows : rows + HEAD_DIM, :] = w_cross[:, pl.ds(column, 128)]
        out[rows + HEAD_DIM :, :] = w_cross[:, pl.ds(column + 128, 128)]


def combine_kernel(*refs):
    combined(refs[:X], refs[X])


def combine(parts, w_cross=None):
    rows = parts[0].shape[0] - TAIL
    parts = [in_vmem(p) for p in parts]
    if w_cross is None:
        shape = pltpu.VMEM((rows, HEAD_DIM), BF16)
        return [pl.pallas_call(
            combine_kernel, compiler_params=PARAMS, out_shape=shape, in_specs=[VMEM] * X, out_specs=VMEM
        )(*parts)] * TP
    return pl.pallas_call(
        first_combine_kernel,
        compiler_params=PARAMS,
        out_shape=[pltpu.VMEM((rows + 2 * HEAD_DIM, HEAD_DIM), BF16)] * TP,
        in_specs=[VMEM] * (X + 1),
        out_specs=[VMEM] * TP,
    )(*parts, in_vmem(w_cross))


def output_kernel(*refs, part):
    heads, weights, (pool, gate) = refs[:TP], refs[TP : 2 * TP], refs[2 * TP : 2 * TP + 2]
    out, staged, sem = refs[-3:]
    rows = staged.shape[0]
    left = jnp.concatenate([h[:rows, :] for h in heads], axis=1)
    base = weights[0].shape[0] - 2 * HEAD_DIM
    right = [jnp.concatenate([w[base + i * HEAD_DIM : base + (i + 1) * HEAD_DIM, :] for w in weights], axis=0) for i in range(2)]
    cross = jnp.dot(left, jnp.concatenate(right, axis=1), preferred_element_type=F32)
    own = slice(part * rows, (part + 1) * rows)
    staged[...] = (pool[own, :] + gate[own, :] * cross).astype(BF16)
    copy = pltpu.make_async_copy(staged, out.at[pl.ds(part * rows, rows), :], sem)
    copy.start()
    copy.wait()


def output(heads, weights, pool, gate, part, before=None):
    rows = pool.shape[0] // HALVES
    operands = [in_vmem(a) for a in (*heads, *weights, pool, gate)]
    in_specs = [VMEM] * len(operands)
    aliases = {}
    if before is not None:
        aliases = {len(operands): 0}
        operands.append(before)
        in_specs.append(HBM)
    return pl.pallas_call(
        functools.partial(output_kernel, part=part),
        compiler_params=PARAMS,
        out_shape=jax.ShapeDtypeStruct(pool.shape, BF16),
        in_specs=in_specs,
        out_specs=HBM,
        scratch_shapes=[pltpu.VMEM((rows, GROUP_WIDTH), BF16), pltpu.SemaphoreType.DMA(())],
        input_output_aliases=aliases,
    )(*operands)


def per_device(
    tokens,
    passage_ids,
    store,
    mix_gain,
    w_query,
    w_key,
    w_value,
    w_cross_out,
    head_scale,
    w_pool_in,
    w_pool_mix,
    pool_scale,
    gate_weight,
):
    gain, scales, gates = (a.reshape(-1, 128) for a in (mix_gain, pool_scale, gate_weight))

    own_kv = own_passages(store.reshape(-1, store.shape[2]), w_key, w_value)
    near = {0: own_kv}
    for d in (1, 7, 2, 6):
        near[d] = z_shift(own_kv, d)

    tokens, own_kv = lax.optimization_barrier((tokens, own_kv))
    own_q = make_queries(tokens, gain, passage_ids, w_query)
    queries = [own_q]
    for d in range(1, X):
        queries.append(x_shift(own_q, d))
    for d, via, step in ((3, 2, 1), (5, 6, 7), (4, 3, 1)):
        near[d] = z_shift(near[via], step)
    chunks = [near[d] for d in range(Z)]
    for d in range(Z):
        chunks.append(core_swap(near[d]))

    sent = attend(head_scale, queries, chunks)
    back = []
    for part in range(HALVES):
        back.append([])
        for d in range(X):
            back[part].append(x_shift(sent[part][d], -d))
    tokens, w_pool_in, first = lax.optimization_barrier((tokens, w_pool_in, sent[0][0]))
    back[0][0] = first
    pool, gate = mix_pools(tokens, gain, scales, gates, w_pool_in, w_pool_mix)
    out, weights = None, None
    for part in range(HALVES):
        attended = combine(back[part], w_cross_out if part == 0 else None)
        heads = []
        for d in range(TP):
            heads.append(tp_shift(attended[d], d))
        weights = weights or heads
        out = output(heads, weights, pool, gate, part, out)
    return out


def solution(mesh):
    return jax.shard_map(
        per_device,
        mesh=mesh,
        in_specs=(
            P("st", None),
            P("st", None),
            P("st", None, None),
            P(),
            P(None, "tp"),
            P(None, "tp"),
            P(None, "tp"),
            P("tp", None),
            P(),
            P(None, "tp"),
            P(),
            P(),
            P(),
        ),
        out_specs=P("st", "tp"),
        check_vma=False,
    )
```
